32 devices in a mesh: grp: 2 (over y), ep: 4 (over z), tp: 4 (over x, core).
Axes of the slice: x: 2, y: 2, z: 4, core: 2. Of those that a mesh axis runs over, the one named last changes fastest.
Arguments:
- memory_query_rows: bfloat16 [1024, 1024], P(('grp', 'ep'), 'tp'), parts along dimension 0, may hold values from -6 to 6
- memory_key_rows: bfloat16 [1024, 1024], P(('grp', 'ep'), 'tp'), parts along dimension 0, may hold values from -6 to 6
- memory_value_rows: bfloat16 [1024, 1024], P(('grp', 'ep'), 'tp'), parts along dimension 0, may hold values from -6 to 6
- input_gate_log: float32 [8, 1024], P('tp', ('grp', 'ep')), parts along dimension 1, may hold values from -4 to 300
- forget_gate_logits: float32 [8, 1024], P('tp', ('grp', 'ep')), parts along dimension 1
- forget_log_extra: float32 [8, 1024], P('tp', ('grp', 'ep')), parts along dimension 1, may hold values from -1.5 to 0
- memory_output_weight: bfloat16 [1024, 2048], P(None, 'tp'), may hold values from -0.1875 to 0.1875
- second_batch_tokens: bfloat16 [4096, 2048], P(('grp', 'ep', 'tp')), parts along dimension 0, may hold values from -6 to 6
- expert_norm_gain: float32 [2048], replicated, may hold values from 0.1 to 1.9
- routing_expert_index: int32 [4096, 2], P(('grp', 'ep', 'tp')), parts along dimension 0, may hold values from 0 to 3, all different within a row; in each aligned block of 128 rows (0 to 127, 128 to 255, ...) at most 80 rows name the same one
- routing_expert_weight: float32 [4096, 2], P(('grp', 'ep', 'tp')), parts along dimension 0, may hold values from 0.2 to 1
- expert_gate_matrix: bfloat16 [4, 2048, 3584], P('ep', None, 'tp'), may hold values from -0.125 to 0.125
- expert_up_matrix: bfloat16 [4, 2048, 3584], P('ep', None, 'tp'), may hold values from -0.125 to 0.125
- expert_down_matrix: bfloat16 [4, 3584, 2048], P('ep', 'tp'), may hold values from -0.09375 to 0.09375
Outputs:
- mixed_out: bfloat16 [1024, 2048], P(('grp', 'ep'), 'tp'), parts along dimension 0
- expert_out: bfloat16 [4096, 2048], P(('grp', 'ep', 'tp')), parts along dimension 0
The draws below stay inside these ranges and needn't reach their ends.
There are 2 independent parts, one for each index of `grp`. The reference program is written for one: setup_inputs(seed, part) draws one part's arguments, and reference() takes and returns one part's arrays. A program takes and returns all parts, laid end to end along the dimension named above; an argument that names none is the same for every part. Nothing has to cross between parts.
Inputs may be any that keep to these rules, and one draw needn't show every extreme that they name: `routing_expert_index`: within the rows of one device no expert is named by more than 80 rows, a bound that some block reaches; the 2 experts of a row differ.
All inputs are finite; a program needn't handle non-finite values.
Results may differ from the reference program's by a relative error of at most 0.012.
The reference program's roundings to bfloat16 on the way count: a program that leaves them out, or rounds other values in their place, can miss the bound.
Values may be sent and summed in bfloat16 or wider, within the bound.
No kernel may reach another device: no remote copies, remote signals or barrier semaphores. Data moves between devices by JAX's collectives and lax.ppermute only.
A program may use at most 128 MiB of HBM per device.

```python
import math
import jax
import jax.numpy as jnp
import numpy as np
from jax import lax

D = 2048
HM = 8
DH = 128
FFE = 3584
TOP = 2
BLOCK = 128
TOK_A_EP = 128
TOK_B_DEV = 128
SEQ_LEN = 512
TOKENS_B = 2048
EXPERTS = 4
CAP = 80
N_TP = 4


def draw_input_gate_log(key, part):
    keys = jax.random.split(key, 1)
    base = jax.random.truncated_normal(keys[0], -4.0, 4.0, (HM, SEQ_LEN), jnp.float32)
    return base.astype(jnp.float32)


def draw_forget_gate_logits(key, part):
    keys = jax.random.split(key, 4)
    threshold = 0.5
    fast = jax.random.uniform(keys[0], (HM,), jnp.float32) < threshold
    fast_rate = 1.0 / jax.random.uniform(keys[1], (HM,), jnp.float32, 30.0, 100.0)
    slow_rate = 0.3 / SEQ_LEN
    rate = jnp.where(fast, fast_rate, slow_rate)
    factor = jnp.exp(jax.random.uniform(keys[2], (HM, SEQ_LEN // TOK_A_EP), jnp.float32, -0.7, 0.7))
    factor = jnp.repeat(factor, TOK_A_EP, axis=1)
    noise = 0.5 * jax.random.truncated_normal(keys[3], -4.0, 4.0, (HM, SEQ_LEN), jnp.float32)
    return (-jnp.log(jnp.expm1(rate[:, None] * factor)) + noise).astype(jnp.float32)


def draw_forget_log_extra(key, part):
    keys = jax.random.split(key, 2)
    places = jax.random.randint(keys[0], (HM, 3), 0, SEQ_LEN)
    amounts = jnp.log(jax.random.uniform(keys[1], (HM, 3), jnp.float32, 0.5, 0.8))
    spots = jnp.arange(SEQ_LEN, dtype=jnp.int32)[None, :]
    result = jnp.zeros((HM, SEQ_LEN), jnp.float32)
    for column in range(3):
        result = result + jnp.where(spots == places[:, column:column + 1], amounts[:, column:column + 1], 0.0)
    return result.astype(jnp.float32)


def block_levels(own_key, shape, cuts, low, top_value):
    loudness, own = 1.0, jax.random.fold_in(own_key, 6)
    for axis_at, parts in cuts:
        draws = jnp.exp(jax.random.uniform(jax.random.fold_in(own, axis_at), (parts,), jnp.float32, low / len(cuts), top_value / len(cuts)))
        loudness = loudness * jnp.repeat(draws, shape[axis_at] // parts).reshape([-1 if axis == axis_at else 1 for axis in range(len(shape))])
    return loudness


def shared_out(own_key, own, number, rows, amount, top, reach, lean):
    sequence = jax.random.permutation(own_key, amount)
    packed, usual = load_shares(amount, rows * top, reach, lean, True), load_shares(amount, rows * top, reach, lean, False)
    places = jnp.arange(amount)

    def named(lengths, offset_by):
        used = int((lengths > 0).sum())
        fixed = max(1, used // 4)
        passed = fixed + (places - fixed + offset_by * (used - fixed)) % max(1, amount - fixed)
        return jnp.zeros((amount,), jnp.int32).at[sequence[jnp.where(places < fixed, places, passed)]].set(jnp.asarray(lengths, jnp.int32))

    lengths = jnp.where(number % 4 == 0, named(packed, number // 4), named(usual, number - number // 4 - 1))
    mixed = jax.random.permutation(jax.random.fold_in(own, 3), amount)
    giver, sink = mixed[0:amount // 2 * 2:2], mixed[1:amount // 2 * 2:2]
    margin = jnp.minimum(lengths[giver] - 1, reach - lengths[sink]) // 2
    margin = jnp.where((giver == sequence[0]) | (sink == sequence[0]) | (lengths[sink] == 0), 0, jnp.maximum(margin, 0))
    passed = jax.random.randint(jax.random.fold_in(own, 4), (amount // 2,), 0, 1 << 20) % (margin + 1)
    lengths = lengths.at[giver].add(-passed).at[sink].add(passed)
    items = jnp.searchsorted(jnp.cumsum(lengths), jnp.arange(rows * top), side="right").astype(jnp.int32)
    grid = items.reshape(top, rows).T
    grid = grid[jax.random.permutation(jax.random.fold_in(own, 1), rows)]
    offset_by = jax.random.randint(jax.random.fold_in(own, 2), (rows, 1), 0, top)
    return jnp.take_along_axis(grid, (jnp.arange(top)[None, :] + offset_by) % top, axis=1)


def load_shares(count, total, reach, lean, full):
    loads = [(1 << 20) // math.isqrt(rank ** lean) + 1 for rank in range(1, count + 1)]
    largest = reach if full else min(reach, max(-(-total // count), total * loads[0] // sum(loads)))
    least = 1 if total - largest >= count - 1 else 0
    given, spare = [largest] + [least] * (count - 1), total - largest - least * (count - 1)
    while spare > 0:
        free = [i for i in range(1, count) if given[i] < largest] or [i for i in range(1, count) if given[i] < reach]
        whole, left = sum([loads[i] for i in free]), spare
        for i in free:
            addition = min(reach - given[i], max(1, left * loads[i] // whole), spare)
            given[i] = given[i] + addition
            spare = spare - addition
    return np.array(given)


def bell_draw(key, dims, scale, bound, pieces=(), held_as=jnp.bfloat16):
    values = jax.random.normal(key, dims, jnp.float32) * scale
    if len(pieces) > 0:
        values = block_levels(key, dims, pieces, -0.22, 0.18) * values
    return jnp.clip(values, min=-bound, max=bound).astype(held_as)


def setup_inputs(seed: int = 0, part: int = 0) -> dict:
    seeds = jax.random.split(jax.random.key(seed), 15)
    part_splits = jax.random.split(jax.random.fold_in(seeds[14], part), 15)
    memory_query_rows = bell_draw(part_splits[0], (SEQ_LEN, HM * DH), 1.0, 6.0, ((0, 4), (1, 4)))
    memory_key_rows = bell_draw(part_splits[1], (SEQ_LEN, HM * DH), 1.0, 6.0, ((0, 4), (1, 4)))
    memory_value_rows = bell_draw(part_splits[2], (SEQ_LEN, HM * DH), 1.0, 6.0, ((0, 4), (1, 4)))
    input_gate_log = draw_input_gate_log(jax.random.fold_in(jax.random.fold_in(seeds[14], part), 71), part)
    forget_gate_logits = draw_forget_gate_logits(jax.random.fold_in(jax.random.fold_in(seeds[14], part), 71), part)
    forget_log_extra = draw_forget_log_extra(jax.random.fold_in(jax.random.fold_in(seeds[14], part), 71), part)
    memory_output_weight = bell_draw(seeds[6], (HM * DH, D), (HM * DH) ** -0.5, 0.1875, ((1, 4),))
    second_batch_tokens = bell_draw(part_splits[7], (TOKENS_B, D), 1.0, 6.0, ((0, 16),))
    expert_norm_gain = jnp.clip(1.0 + 0.18 * jax.random.normal(seeds[8], (D,), jnp.float32), 0.1, 1.9)
    routing_expert_index_keys = jax.random.split(jax.random.fold_in(part_splits[9], 1), TOKENS_B // TOK_B_DEV)
    routing_expert_index_turns = jax.random.permutation(jax.random.fold_in(part_splits[9], 3), TOKENS_B // TOK_B_DEV)
    routing_expert_index = jax.vmap(lambda own, number: shared_out(jax.random.fold_in(part_splits[9], 2), own, number, TOK_B_DEV, EXPERTS, TOP, CAP, 1))(routing_expert_index_keys, routing_expert_index_turns).reshape((TOKENS_B, TOP))
    routing_expert_weight = jnp.clip(0.2 + 0.8 * jax.random.uniform(part_splits[10], (TOKENS_B, TOP), jnp.float32) ** block_levels(part_splits[10], (TOKENS_B, TOP), ((0, 16),), -0.2, 0.2), 0.2, 1.0)
    expert_gate_matrix = bell_draw(seeds[11], (EXPERTS, D, FFE), D ** -0.5, 0.125, ((0, 4), (2, 4)))
    expert_up_matrix = bell_draw(seeds[12], (EXPERTS, D, FFE), D ** -0.5, 0.125, ((0, 4), (2, 4)))
    expert_down_matrix = bell_draw(seeds[13], (EXPERTS, FFE, D), FFE ** -0.5, 0.09375, ((0, 4), (1, 4)))
    return {"memory_query_rows": memory_query_rows, "memory_key_rows": memory_key_rows, "memory_value_rows": memory_value_rows, "input_gate_log": input_gate_log, "forget_gate_logits": forget_gate_logits, "forget_log_extra": forget_log_extra, "memory_output_weight": memory_output_weight, "second_batch_tokens": second_batch_tokens, "expert_norm_gain": expert_norm_gain, "routing_expert_index": routing_expert_index, "routing_expert_weight": routing_expert_weight, "expert_gate_matrix": expert_gate_matrix, "expert_up_matrix": expert_up_matrix, "expert_down_matrix": expert_down_matrix}


rms_eps = 1e-06
highest = lax.Precision.HIGHEST

def state_update(state_in, inputs, cumulative):
    memory, normer, stabilizer = state_in
    key_rows, values, in_gate, forget = inputs
    block_total = cumulative[:, -1]
    weights = block_total[:, None] - cumulative + in_gate
    new_stab = jnp.maximum(block_total + stabilizer, lax.optimization_barrier(jnp.max(weights, axis=-1)))
    scaled = jnp.exp(weights - new_stab[:, None])
    retained = jnp.exp(block_total + stabilizer - new_stab)
    weighted_keys = scaled[:, :, None] * key_rows
    memory = retained[:, None, None] * memory + jnp.einsum('hsd,hse->hde', weighted_keys, values, precision=highest)
    normer = retained[:, None] * normer + lax.optimization_barrier(jnp.sum(weighted_keys, axis=1))
    return (memory, normer, new_stab)

def block_step(state_in, inputs):
    memory, normer, stabilizer = state_in
    queries, key_rows, values, in_gate, forget = inputs
    length = queries.shape[1]
    causal = jnp.tril(jnp.ones((length, length), dtype=bool))
    cumulative = jnp.cumsum(forget, axis=-1)
    decays = jnp.where(causal, cumulative[:, :, None] - cumulative[:, None, :] + in_gate[:, None, :], -jnp.inf)
    carried_max = cumulative + stabilizer[:, None]
    row_max = jnp.maximum(lax.optimization_barrier(jnp.max(decays, axis=-1)), carried_max)
    scores = jnp.einsum('htd,hsd->hts', queries, key_rows, precision=highest) * jnp.exp(decays - row_max[:, :, None])
    carried = jnp.exp(carried_max - row_max)
    numerator = carried[:, :, None] * jnp.einsum('htd,hde->hte', queries, memory, precision=highest) + jnp.einsum('hts,hse->hte', scores, values, precision=highest)
    denominator = carried * jnp.einsum('htd,hd->ht', queries, normer, precision=highest) + lax.optimization_barrier(jnp.sum(scores, axis=-1))
    output = numerator / jnp.maximum(jnp.abs(denominator), jnp.exp(-row_max))[:, :, None]
    new_state = state_update(state_in, (key_rows, values, in_gate, forget), cumulative)
    return (new_state, output)

def split_blocks(row_block, heads):
    count = row_block.shape[0] // BLOCK
    return row_block.astype(jnp.float32).reshape(count, BLOCK, heads, -1).transpose(0, 2, 1, 3)

def gate_blocks(gate_rows):
    heads = gate_rows.shape[0]
    return gate_rows.reshape(heads, -1, BLOCK).transpose(1, 0, 2)

def expert_ffn(row_block, gate_weight, up_weight, down_weight):
    gate_act = jnp.dot(row_block, gate_weight, preferred_element_type=jnp.float32)
    up_act = jnp.dot(row_block, up_weight, preferred_element_type=jnp.float32)
    hidden = (jax.nn.silu(gate_act) * up_act).astype(jnp.bfloat16)
    group_width = FFE // N_TP
    running = jnp.zeros((row_block.shape[0], D), jnp.float32)
    for group in range(N_TP):
        part_rows = hidden[:, group * group_width:(group + 1) * group_width]
        part_down = down_weight[group * group_width:(group + 1) * group_width]
        partial_out = jnp.dot(part_rows, part_down, preferred_element_type=jnp.float32).astype(jnp.bfloat16)
        running = running + partial_out.astype(jnp.float32)
    return running.astype(jnp.bfloat16)

def reference(memory_query_rows, memory_key_rows, memory_value_rows, input_gate_log, forget_gate_logits, forget_log_extra, memory_output_weight, second_batch_tokens, expert_norm_gain, routing_expert_index, routing_expert_weight, expert_gate_matrix, expert_up_matrix, expert_down_matrix):
    queries = split_blocks(memory_query_rows, HM)
    key_rows = split_blocks(memory_key_rows, HM) * DH ** (-0.5)
    values = split_blocks(memory_value_rows, HM)
    forget_log_value = jax.nn.log_sigmoid(forget_gate_logits) + forget_log_extra
    start_state = (jnp.zeros((HM, DH, DH), jnp.float32), jnp.zeros((HM, DH), jnp.float32), jnp.zeros((HM,), jnp.float32))
    _, outputs = lax.scan(block_step, start_state, (queries, key_rows, values, gate_blocks(input_gate_log), gate_blocks(forget_log_value)))
    memory_rows = outputs.transpose(0, 2, 1, 3).reshape(SEQ_LEN, HM * DH).astype(jnp.bfloat16)
    mixed_out = jnp.dot(memory_rows, memory_output_weight, preferred_element_type=jnp.float32).astype(jnp.bfloat16)
    tokens_f = second_batch_tokens.astype(jnp.float32)
    normed = (tokens_f * lax.rsqrt(lax.optimization_barrier(jnp.mean(tokens_f * tokens_f, axis=1, keepdims=True)) + rms_eps) * expert_norm_gain).astype(jnp.bfloat16)
    devices = TOKENS_B // TOK_B_DEV
    flat_ids = routing_expert_index.reshape(devices, TOK_B_DEV * TOP)
    onehot = (flat_ids[:, :, None] == jnp.arange(EXPERTS, dtype=jnp.int32)[None, None, :]).astype(jnp.int32)
    route_ranks = lax.optimization_barrier(jnp.sum((jnp.cumsum(onehot, axis=1) - 1) * onehot, axis=2))
    owner = jnp.arange(devices, dtype=jnp.int32)[:, None]
    slot_ids = (flat_ids * (devices * CAP) + owner * CAP + route_ranks).reshape(-1).astype(jnp.int32)
    token_ids = jnp.repeat(jnp.arange(TOKENS_B, dtype=jnp.int32), TOP)
    slot_table = jnp.full((EXPERTS * devices * CAP,), TOKENS_B, jnp.int32).at[slot_ids].set(token_ids)
    padded = jnp.concatenate([normed, jnp.zeros((1, D), jnp.bfloat16)], axis=0)

    def one_expert(inputs):
        index_rows, gate_weight, up_weight, down_weight = inputs
        return expert_ffn(padded[index_rows], gate_weight, up_weight, down_weight)
    results = lax.map(one_expert, (slot_table.reshape(EXPERTS, devices * CAP), expert_gate_matrix, expert_up_matrix, expert_down_matrix))
    picked = results.reshape(-1, D)[slot_ids].astype(jnp.float32).reshape(TOKENS_B, TOP, D)
    expert_out = lax.optimization_barrier(jnp.sum(picked * routing_expert_weight[:, :, None], axis=1)).astype(jnp.bfloat16)
    return (mixed_out, expert_out)
```

```python
import jax
import jax.numpy as jnp
from jax import lax
from jax.sharding import PartitionSpec as P

DH = 128
TOP = 2
BLOCK = 128


neg_big = -1e30
rms_eps = 1e-06
highest = lax.Precision.HIGHEST


def entering(part, axis, combine, identity):
    place = lax.axis_index(axis)
    gathered = jax.tree.map(lambda a: lax.all_gather(a, axis), part)
    state = jax.tree.map(lambda a, e: jnp.zeros_like(a) + jnp.asarray(e, a.dtype), part, identity)

    def one(turn, state):
        return combine(
            state, jax.tree.map(lambda a: lax.dynamic_index_in_dim(a, turn, 0, False), gathered)
        )

    return lax.fori_loop(0, place, one, state)


def entering_chain(local_state, total, axis):
    mem_local, norm_local, stab_local = local_state
    size = lax.axis_size(axis)

    def pack(memory, normer, stabilizer):
        stab_row = jnp.broadcast_to(stabilizer[:, None, None], (memory.shape[0], 1, memory.shape[2]))
        return jnp.concatenate([memory, normer[:, None, :], stab_row], axis=1)

    def unpack(packed):
        rows = mem_local.shape[1]
        return (packed[:, :rows], packed[:, rows], packed[:, rows + 1, 0])

    packed = jnp.zeros_like(pack(*local_state))
    for hop in range(size - 1):
        after = pack(*join_states(unpack(packed), local_state, total))
        packed = packed + lax.ppermute(after, axis, [(hop, hop + 1)])
    return unpack(packed)


def state_update(state_in, inputs, cumulative):
    memory, normer, stabilizer = state_in
    key_rows, values, in_gate, forget = inputs
    block_total = cumulative[:, -1]
    weights = block_total[:, None] - cumulative + in_gate
    new_stab = jnp.maximum(block_total + stabilizer, jnp.max(weights, axis=-1))
    scaled = jnp.exp(weights - new_stab[:, None])
    retained = jnp.exp(block_total + stabilizer - new_stab)
    weighted_keys = scaled[:, :, None] * key_rows
    memory = retained[:, None, None] * memory + jnp.einsum(
        "hsd,hse->hde", weighted_keys, values, precision=highest
    )
    normer = retained[:, None] * normer + jnp.sum(weighted_keys, axis=1)
    return (memory, normer, new_stab)


def block_step(state_in, inputs, cumulative):
    memory, normer, stabilizer = state_in
    queries, key_rows, values, in_gate, forget = inputs
    length = queries.shape[1]
    causal = jnp.tril(jnp.ones((length, length), dtype=bool))
    decays = jnp.where(
        causal, cumulative[:, :, None] - cumulative[:, None, :] + in_gate[:, None, :], -jnp.inf
    )
    carried_max = cumulative + stabilizer[:, None]
    row_max = jnp.maximum(jnp.max(decays, axis=-1), carried_max)
    scores = jnp.einsum("htd,hsd->hts", queries, key_rows, precision=highest) * jnp.exp(
        decays - row_max[:, :, None]
    )
    carried = jnp.exp(carried_max - row_max)
    numerator = carried[:, :, None] * jnp.einsum(
        "htd,hde->hte", queries, memory, precision=highest
    ) + jnp.einsum("hts,hse->hte", scores, values, precision=highest)
    denominator = carried * jnp.einsum("htd,hd->ht", queries, normer, precision=highest) + jnp.sum(
        scores, axis=-1
    )
    return numerator / jnp.maximum(jnp.abs(denominator), jnp.exp(-row_max))[:, :, None]


def join_states(earlier, later, total_late):
    mem_early, norm_early, stab_early = earlier
    mem_late, norm_late, stab_late = later
    stabilizer = jnp.maximum(total_late + stab_early, stab_late)
    early_scale = jnp.exp(total_late + stab_early - stabilizer)
    late_scale = jnp.exp(stab_late - stabilizer)
    memory = early_scale[:, None, None] * mem_early + late_scale[:, None, None] * mem_late
    normer = early_scale[:, None] * norm_early + late_scale[:, None] * norm_late
    return (memory, normer, stabilizer)


def join_totals(earlier, later):
    joined = join_states(earlier[:3], later[:3], later[3])
    return joined + (earlier[3] + later[3],)


def split_blocks(row_block, heads):
    count = row_block.shape[0] // BLOCK
    return row_block.astype(jnp.float32).reshape(count, BLOCK, heads, -1).transpose(0, 2, 1, 3)


def gate_blocks(gate_rows):
    heads = gate_rows.shape[0]
    return gate_rows.reshape(heads, -1, BLOCK).transpose(1, 0, 2)


def swap(rows, axis, bit):
    size = lax.axis_size(axis)
    return lax.ppermute(rows, axis, [(i, i ^ bit) for i in range(size)])


def tp_bits():
    size = lax.axis_size("tp")
    bits = []
    while size > 1:
        size //= 2
        bits.append(size)
    return bits


def gather_near(rows):
    for bit in tp_bits():
        rows = jnp.concatenate([rows, swap(rows, "tp", bit)], axis=0)
    return rows


def scatter_near(parts):
    for bit in reversed(tp_bits()):
        half = parts.shape[0] // 2
        away = parts[half:].astype(jnp.bfloat16)
        parts = parts[:half] + swap(away, "tp", bit).astype(jnp.float32)
    return parts


def gather_columns(rows):
    place = lax.axis_index("tp")
    for bit in reversed(tp_bits()):
        other = swap(rows, "tp", bit)
        upper = (place & bit) != 0
        rows = jnp.concatenate(
            [jnp.where(upper, other, rows), jnp.where(upper, rows, other)], axis=1
        )
    return rows


def memory_branch(
    memory_query_rows,
    memory_key_rows,
    memory_value_rows,
    input_gate_log,
    forget_gate_logits,
    forget_log_extra,
    memory_output_weight,
    chained,
):
    heads_local, positions = input_gate_log.shape
    queries = split_blocks(memory_query_rows, heads_local)
    key_rows = split_blocks(memory_key_rows, heads_local) * DH ** (-0.5)
    values = split_blocks(memory_value_rows, heads_local)
    in_gate = gate_blocks(input_gate_log)
    forget_log_value = jax.nn.log_sigmoid(forget_gate_logits) + forget_log_extra
    forget = gate_blocks(forget_log_value)
    upto = jnp.triu(jnp.ones((BLOCK, BLOCK), jnp.float32))
    cumulative = jnp.einsum("bhs,st->bht", forget, upto, precision=highest)
    zero_memory = jnp.zeros((heads_local, DH, DH), jnp.float32)
    zero_normer = jnp.zeros((heads_local, DH), jnp.float32)
    low_stab = jnp.full((heads_local,), neg_big, jnp.float32)
    count = positions // BLOCK
    state = (zero_memory, zero_normer, low_stab)
    for b in range(count):
        state = state_update(state, (key_rows[b], values[b], in_gate[b], forget[b]), cumulative[b])
    totals = jnp.sum(cumulative[:, :, -1], axis=0)
    if chained:
        incoming = entering_chain(state, totals, "ep")
    else:
        identity = (zero_memory, zero_normer, low_stab, jnp.zeros((heads_local,), jnp.float32))
        mem_prior, norm_prior, stab_prior, total_prior = entering(
            state + (totals,), "ep", join_totals, identity
        )
        stab_in = jnp.maximum(total_prior, stab_prior)
        factor = jnp.exp(stab_prior - stab_in)
        incoming = (factor[:, None, None] * mem_prior, factor[:, None] * norm_prior, stab_in)
    outputs = []
    for b in range(count):
        block = (queries[b], key_rows[b], values[b], in_gate[b], forget[b])
        outputs.append(block_step(incoming, block, cumulative[b]))
        if b + 1 < count:
            incoming = state_update(incoming, block[1:], cumulative[b])
    memory_rows = (
        jnp.stack(outputs).transpose(0, 2, 1, 3).reshape(positions, -1).astype(jnp.bfloat16)
    )
    mixed = jnp.dot(
        gather_columns(memory_rows), memory_output_weight, preferred_element_type=jnp.float32
    )
    return mixed.astype(jnp.bfloat16)


def expert_part(rows, gate_weight, up_weight, down_weight):
    gate_act = jnp.dot(rows, gate_weight, preferred_element_type=jnp.float32)
    up_act = jnp.dot(rows, up_weight, preferred_element_type=jnp.float32)
    hidden = (jax.nn.silu(gate_act) * up_act).astype(jnp.bfloat16)
    return jnp.dot(hidden, down_weight, preferred_element_type=jnp.float32)


def expert_branch(
    second_batch_tokens,
    expert_norm_gain,
    routing_expert_index,
    routing_expert_weight,
    gate_weight,
    up_weight,
    down_weight,
    paired,
):
    tok_rows = second_batch_tokens.shape[0]
    experts = lax.axis_size("ep")
    capacity = max(2, 5 * tok_rows * TOP // (4 * experts))
    place = lax.axis_index("ep")
    tokens_f = second_batch_tokens.astype(jnp.float32)
    normed = (
        tokens_f
        * lax.rsqrt(jnp.mean(tokens_f * tokens_f, axis=1, keepdims=True) + rms_eps)
        * expert_norm_gain
    ).astype(jnp.bfloat16)
    if paired:
        ids = place ^ jnp.arange(experts, dtype=jnp.int32)
    else:
        ids = jnp.arange(experts, dtype=jnp.int32)
    hits = routing_expert_index[:, :, None] == ids[None, None, :]
    named = jnp.any(hits, axis=1)
    share = jnp.sum(jnp.where(hits, routing_expert_weight[:, :, None], 0.0), axis=1)
    upto = jnp.tril(jnp.ones((tok_rows, tok_rows), jnp.bfloat16))
    ranks = jnp.dot(upto, named.astype(jnp.bfloat16), preferred_element_type=jnp.float32)
    slot = jnp.where(named, ranks.astype(jnp.int32) - 1, -1)
    table = jnp.arange(capacity, dtype=jnp.int32)
    placing = (slot.T[:, None, :] == table[None, :, None]).astype(jnp.bfloat16)
    combine = jnp.where(slot[:, :, None] == table[None, None, :], share[:, :, None], 0.0)
    weights = (gate_weight, up_weight, down_weight)
    if paired:
        returned = [None] * experts
        for k in reversed(range(experts)):
            rows = jnp.dot(placing[k], normed, preferred_element_type=jnp.float32)
            rows = rows.astype(jnp.bfloat16)
            if k:
                rows = swap(rows, "ep", k)
            parts = expert_part(gather_near(rows), *weights)
            summed = scatter_near(parts).astype(jnp.bfloat16)
            if k:
                summed = swap(summed, "ep", k)
            returned[k] = summed
        returned = jnp.concatenate(returned, axis=0)
    else:
        outgoing = jnp.dot(
            placing.reshape(experts * capacity, tok_rows),
            normed,
            preferred_element_type=jnp.float32,
        ).astype(jnp.bfloat16)
        arrived = lax.all_to_all(outgoing, "ep", split_axis=0, concat_axis=0, tiled=True)
        row_block = lax.all_gather(arrived, "tp", axis=0, tiled=True)
        terms = expert_part(row_block, *weights).astype(jnp.bfloat16)
        summed = lax.psum_scatter(terms, "tp", scatter_dimension=0, tiled=True)
        returned = lax.all_to_all(summed, "ep", split_axis=0, concat_axis=0, tiled=True)
    combine = combine.reshape(tok_rows, experts * capacity)
    high = combine.astype(jnp.bfloat16)
    low = (combine - high.astype(jnp.float32)).astype(jnp.bfloat16)
    both = jnp.dot(
        jnp.concatenate([high, low], axis=0), returned, preferred_element_type=jnp.float32
    )
    return (both[:tok_rows] + both[tok_rows:]).astype(jnp.bfloat16)


def on_device(
    memory_query_rows,
    memory_key_rows,
    memory_value_rows,
    input_gate_log,
    forget_gate_logits,
    forget_log_extra,
    memory_output_weight,
    second_batch_tokens,
    expert_norm_gain,
    routing_expert_index,
    routing_expert_weight,
    expert_gate_matrix,
    expert_up_matrix,
    expert_down_matrix,
):
    experts = lax.axis_size("ep")
    paired = experts <= 8 and experts & (experts - 1) == 0
    expert_out = expert_branch(
        second_batch_tokens,
        expert_norm_gain,
        routing_expert_index,
        routing_expert_weight,
        expert_gate_matrix[0],
        expert_up_matrix[0],
        expert_down_matrix[0],
        paired,
    )
    mixed_out = memory_branch(
        memory_query_rows,
        memory_key_rows,
        memory_value_rows,
        input_gate_log,
        forget_gate_logits,
        forget_log_extra,
        memory_output_weight,
        paired,
    )
    return (mixed_out, expert_out)


def solution(mesh):
    placed = (
        P(("grp", "ep"), "tp"),
        P(("grp", "ep"), "tp"),
        P(("grp", "ep"), "tp"),
        P("tp", ("grp", "ep")),
        P("tp", ("grp", "ep")),
        P("tp", ("grp", "ep")),
        P(None, "tp"),
        P(("grp", "ep", "tp"), None),
        P(),
        P(("grp", "ep", "tp"), None),
        P(("grp", "ep", "tp"), None),
        P("ep", None, "tp"),
        P("ep", None, "tp"),
        P("ep", "tp", None),
    )
    return jax.shard_map(
        on_device,
        mesh=mesh,
        in_specs=placed,
        out_specs=(P(("grp", "ep"), "tp"), P(("grp", "ep", "tp"), None)),
        check_vma=False,
    )
```

```python
import jax
import jax.numpy as jnp
from jax import lax
from jax.experimental import pallas as pl
from jax.experimental.pallas import tpu as pltpu
from jax.sharding import PartitionSpec as P

DH = 128
TOP = 2
BLOCK = 128


neg_big = -1e30
rms_eps = 1e-06
highest = lax.Precision.HIGHEST


def entering(part, axis, combine, identity):
    place = lax.axis_index(axis)
    gathered = jax.tree.map(lambda a: lax.all_gather(a, axis), part)
    state = jax.tree.map(lambda a, e: jnp.zeros_like(a) + jnp.asarray(e, a.dtype), part, identity)

    def one(turn, state):
        return combine(
            state, jax.tree.map(lambda a: lax.dynamic_index_in_dim(a, turn, 0, False), gathered)
        )

    return lax.fori_loop(0, place, one, state)


def state_update(state_in, inputs, cumulative):
    memory, normer, stabilizer = state_in
    key_rows, values, in_gate, _ = inputs
    block_total = cumulative[:, -1]
    weights = block_total[:, None] - cumulative + in_gate
    new_stab = jnp.maximum(block_total + stabilizer, jnp.max(weights, axis=-1))
    scaled = jnp.exp(weights - new_stab[:, None])
    retained = jnp.exp(block_total + stabilizer - new_stab)
    weighted_keys = scaled[:, :, None] * key_rows
    memory = retained[:, None, None] * memory + jnp.einsum(
        "hsd,hse->hde", weighted_keys, values, precision=highest
    )
    normer = retained[:, None] * normer + jnp.sum(weighted_keys, axis=1)
    return (memory, normer, new_stab)


def block_step(state_in, inputs, cumulative):
    memory, normer, stabilizer = state_in
    queries, key_rows, values, in_gate, _ = inputs
    length = queries.shape[1]
    causal = jnp.tril(jnp.ones((length, length), dtype=bool))
    decays = jnp.where(
        causal, cumulative[:, :, None] - cumulative[:, None, :] + in_gate[:, None, :], -jnp.inf
    )
    carried_max = cumulative + stabilizer[:, None]
    row_max = jnp.maximum(jnp.max(decays, axis=-1), carried_max)
    scores = jnp.einsum("htd,hsd->hts", queries, key_rows, precision=highest) * jnp.exp(
        decays - row_max[:, :, None]
    )
    carried = jnp.exp(carried_max - row_max)
    numerator = carried[:, :, None] * jnp.einsum(
        "htd,hde->hte", queries, memory, precision=highest
    ) + jnp.einsum("hts,hse->hte", scores, values, precision=highest)
    denominator = carried * jnp.einsum("htd,hd->ht", queries, normer, precision=highest) + jnp.sum(
        scores, axis=-1
    )
    return numerator / jnp.maximum(jnp.abs(denominator), jnp.exp(-row_max))[:, :, None]


def join_states(earlier, later, total_late):
    mem_early, norm_early, stab_early = earlier
    mem_late, norm_late, stab_late = later
    stabilizer = jnp.maximum(total_late + stab_early, stab_late)
    early_scale = jnp.exp(total_late + stab_early - stabilizer)
    late_scale = jnp.exp(stab_late - stabilizer)
    memory = early_scale[:, None, None] * mem_early + late_scale[:, None, None] * mem_late
    normer = early_scale[:, None] * norm_early + late_scale[:, None] * norm_late
    return (memory, normer, stabilizer)


def join_totals(earlier, later):
    joined = join_states(earlier[:3], later[:3], later[3])
    return joined + (earlier[3] + later[3],)


def split_blocks(row_block, heads):
    count = row_block.shape[0] // BLOCK
    return row_block.astype(jnp.float32).reshape(count, BLOCK, heads, -1).transpose(0, 2, 1, 3)


def gate_blocks(gate_rows):
    heads = gate_rows.shape[0]
    return gate_rows.reshape(heads, -1, BLOCK).transpose(1, 0, 2)


def swap(rows, axis, bit):
    size = lax.axis_size(axis)
    return lax.ppermute(rows, axis, [(i, i ^ bit) for i in range(size)])


def tp_bits():
    size = lax.axis_size("tp")
    bits = []
    while size > 1:
        size //= 2
        bits.append(size)
    return bits


def gather_columns(rows):
    place = lax.axis_index("tp")
    for bit in reversed(tp_bits()):
        other = swap(rows, "tp", bit)
        upper = (place & bit) != 0
        rows = jnp.concatenate(
            [jnp.where(upper, other, rows), jnp.where(upper, rows, other)], axis=1
        )
    return rows


def memory_branch(
    memory_query_rows,
    memory_key_rows,
    memory_value_rows,
    input_gate_log,
    forget_gate_logits,
    forget_log_extra,
    memory_output_weight,
):
    heads_local, positions = input_gate_log.shape
    queries = split_blocks(memory_query_rows, heads_local)
    key_rows = split_blocks(memory_key_rows, heads_local) * DH ** (-0.5)
    values = split_blocks(memory_value_rows, heads_local)
    in_gate = gate_blocks(input_gate_log)
    forget_log_value = jax.nn.log_sigmoid(forget_gate_logits) + forget_log_extra
    forget = gate_blocks(forget_log_value)
    upto = jnp.triu(jnp.ones((BLOCK, BLOCK), jnp.float32))
    cumulative = jnp.einsum("bhs,st->bht", forget, upto, precision=highest)
    zero_memory = jnp.zeros((heads_local, DH, DH), jnp.float32)
    zero_normer = jnp.zeros((heads_local, DH), jnp.float32)
    low_stab = jnp.full((heads_local,), neg_big, jnp.float32)
    count = positions // BLOCK
    state = (zero_memory, zero_normer, low_stab)
    for b in range(count):
        state = state_update(state, (key_rows[b], values[b], in_gate[b], forget[b]), cumulative[b])
    totals = jnp.sum(cumulative[:, :, -1], axis=0)
    identity = (zero_memory, zero_normer, low_stab, jnp.zeros((heads_local,), jnp.float32))
    mem_prior, norm_prior, stab_prior, total_prior = entering(
        state + (totals,), "ep", join_totals, identity
    )
    stab_in = jnp.maximum(total_prior, stab_prior)
    factor = jnp.exp(stab_prior - stab_in)
    incoming = (factor[:, None, None] * mem_prior, factor[:, None] * norm_prior, stab_in)
    outputs = []
    for b in range(count):
        block = (queries[b], key_rows[b], values[b], in_gate[b], forget[b])
        outputs.append(block_step(incoming, block, cumulative[b]))
        if b + 1 < count:
            incoming = state_update(incoming, block[1:], cumulative[b])
    memory_rows = (
        jnp.stack(outputs).transpose(0, 2, 1, 3).reshape(positions, -1).astype(jnp.bfloat16)
    )
    mixed = jnp.dot(
        gather_columns(memory_rows), memory_output_weight, preferred_element_type=jnp.float32
    )
    return mixed.astype(jnp.bfloat16)


def split_terms(array):
    high = array.astype(jnp.bfloat16)
    return high, (array - high.astype(jnp.float32)).astype(jnp.bfloat16)


def wide_dot(left, right):
    high, low = split_terms(left)
    both = jnp.dot(
        jnp.concatenate([high, low], axis=0), right, preferred_element_type=jnp.float32
    )
    return both[: left.shape[0]] + both[left.shape[0] :]


def local_kernel(query, key, value, gate, logits, extra, local, after, inside, columns):
    heads = gate.shape[0]
    size = query.shape[0]
    scale = DH ** (-0.5)
    raw = logits[...]
    forget = jnp.minimum(raw, 0.0) - jnp.log1p(jnp.exp(-jnp.abs(raw))) + extra[...]
    first = lax.broadcasted_iota(jnp.int32, (size, size), 0)
    second = lax.broadcasted_iota(jnp.int32, (size, size), 1)
    upto = (first <= second).astype(jnp.float32)
    cumulative = jnp.dot(forget, upto, precision=highest, preferred_element_type=jnp.float32)
    ending = cumulative[:, size - 1 : size] - cumulative + gate[...]
    peak = jnp.max(ending, axis=1, keepdims=True)
    grow = jnp.exp(ending - peak)
    blank = jnp.zeros((size - 2 * heads, size), jnp.float32)
    turned = jnp.concatenate([cumulative, grow, blank], axis=0).T
    notes = [jnp.zeros((size, size - 3 * heads), jnp.float32)]
    for h in range(heads):
        span = slice(h * DH, (h + 1) * DH)
        queries = query[:, span]
        keys = key[:, span]
        values = value[:, span]
        keys_f = keys.astype(jnp.float32) * scale
        weighted = keys_f.T * grow[h : h + 1, :]
        memory = wide_dot(weighted, values)
        normer = jnp.sum(keys_f * turned[:, heads + h : heads + h + 1], axis=0, keepdims=True)
        total = cumulative[h : h + 1, size - 1 : size]
        stab = peak[h : h + 1, :]
        later = jnp.maximum(total, stab)
        ratio = jnp.exp(stab - later)
        local[h, 0:DH, :] = memory
        local[h, DH : DH + 1, :] = normer
        local[h, DH + 1 : DH + 2, :] = jnp.broadcast_to(stab, (1, DH))
        local[h, DH + 2 : DH + 3, :] = jnp.broadcast_to(total, (1, DH))
        after[h, 0:DH, :] = memory * ratio
        after[h, DH : DH + 1, :] = normer * ratio
        after[h, DH + 1 : DH + 2, :] = jnp.broadcast_to(later, (1, DH))
        column = turned[:, h : h + 1]
        decays = column - cumulative[h : h + 1, :] + gate[h : h + 1, :]
        decays = jnp.where(second <= first, decays, -jnp.inf)
        row_max = jnp.max(decays, axis=1, keepdims=True)
        scores = lax.dot_general(
            queries, keys, (((1,), (1,)), ((), ())), preferred_element_type=jnp.float32
        )
        scores = scores * scale * jnp.exp(decays - row_max)
        inside[:, span] = wide_dot(scores, values)
        notes = notes[:-1] + [column, row_max, jnp.sum(scores, axis=1, keepdims=True)] + notes[-1:]
    columns[...] = jnp.concatenate(notes, axis=1)


def join_kernel(local, *refs):
    earlier = refs[:-1]
    after = refs[-1]
    for h in range(local.shape[0]):
        entering = sum(part[h] for part in earlier)
        stab = entering[DH + 1 : DH + 2, :] + local[h, DH + 2 : DH + 3, :]
        late = local[h, DH + 1 : DH + 2, :]
        later = jnp.maximum(stab, late)
        keep = jnp.exp(stab - later)
        grow = jnp.exp(late - later)
        after[h, 0 : DH + 1, :] = entering[0 : DH + 1, :] * keep + local[h, 0 : DH + 1, :] * grow
        after[h, DH + 1 : DH + 2, :] = later


def output_kernel(query, inside, columns, *refs):
    earlier = refs[:-1]
    out = refs[-1]
    for h in range(earlier[0].shape[0]):
        span = slice(h * DH, (h + 1) * DH)
        entering = sum(part[h] for part in earlier)
        queries = query[:, span]
        high, low = split_terms(entering[0:DH, :])
        carried = jnp.dot(queries, high, preferred_element_type=jnp.float32) + jnp.dot(
            queries, low, preferred_element_type=jnp.float32
        )
        normed = jnp.sum(
            queries.astype(jnp.float32) * entering[DH : DH + 1, :], axis=1, keepdims=True
        )
        arrived = columns[:, 3 * h : 3 * h + 1] + entering[DH + 1 : DH + 2, 0:1]
        row_max = columns[:, 3 * h + 1 : 3 * h + 2]
        top = jnp.maximum(row_max, arrived)
        outer = jnp.exp(arrived - top)
        inner = jnp.exp(row_max - top)
        below = outer * normed + inner * columns[:, 3 * h + 2 : 3 * h + 3]
        above = outer * carried + inner * inside[:, span]
        out[:, span] = (above / jnp.maximum(jnp.abs(below), jnp.exp(-top))).astype(jnp.bfloat16)


def mixed_kernel(place, own, across, beside, corner, weight, out):
    width = own.shape[1]
    total = jnp.zeros(out.shape, jnp.float32)
    for mask, part in ((0, own), (2, across), (1, beside), (3, corner)):
        rows = pl.ds(pl.multiple_of((place[0] ^ mask) * width, width), width)
        total += jnp.dot(part[...], weight[rows, :], preferred_element_type=jnp.float32)
    out[...] = total.astype(jnp.bfloat16)


def memory_pairs(
    memory_query_rows,
    memory_key_rows,
    memory_value_rows,
    input_gate_log,
    forget_gate_logits,
    forget_log_extra,
    memory_output_weight,
):
    heads = input_gate_log.shape[0]
    size, width = memory_query_rows.shape
    vmem = pl.BlockSpec(memory_space=pltpu.VMEM)
    params = pltpu.CompilerParams(vmem_limit_bytes=8 * 1024 * 1024)
    packed = jax.ShapeDtypeStruct((heads, DH + 8, DH), jnp.float32)
    local, after, inside, columns = pl.pallas_call(
        local_kernel,
        in_specs=[vmem] * 6,
        out_specs=[vmem] * 4,
        out_shape=[
            packed,
            packed,
            jax.ShapeDtypeStruct((size, width), jnp.float32),
            jax.ShapeDtypeStruct((size, size), jnp.float32),
        ],
        compiler_params=params,
    )(
        memory_query_rows,
        memory_key_rows,
        memory_value_rows,
        input_gate_log,
        forget_gate_logits,
        forget_log_extra,
    )
    earlier = []
    hops = lax.axis_size("ep") - 1
    for hop in range(hops):
        if hop:
            after = pl.pallas_call(
                join_kernel,
                in_specs=[vmem] * (1 + hop),
                out_specs=vmem,
                out_shape=packed,
                compiler_params=params,
            )(local, *earlier)
        earlier.append(lax.ppermute(after, "ep", [(hop, hop + 1)]))
    own = pl.pallas_call(
        output_kernel,
        in_specs=[vmem] * (3 + hops),
        out_specs=vmem,
        out_shape=jax.ShapeDtypeStruct((size, width), jnp.bfloat16),
        compiler_params=params,
    )(memory_query_rows, inside, columns, *earlier)
    across = swap(own, "tp", 2)
    beside = swap(own, "tp", 1)
    corner = swap(across, "tp", 1)
    place = lax.axis_index("tp").astype(jnp.int32).reshape(1)
    return pl.pallas_call(
        mixed_kernel,
        in_specs=[pl.BlockSpec(memory_space=pltpu.SMEM)] + [vmem] * 5,
        out_specs=vmem,
        out_shape=jax.ShapeDtypeStruct((size, memory_output_weight.shape[1]), jnp.bfloat16),
        compiler_params=params,
    )(place, own, across, beside, corner, memory_output_weight)


def expert_part(rows, gate_weight, up_weight, down_weight):
    gate_act = jnp.dot(rows, gate_weight, preferred_element_type=jnp.float32)
    up_act = jnp.dot(rows, up_weight, preferred_element_type=jnp.float32)
    hidden = (jax.nn.silu(gate_act) * up_act).astype(jnp.bfloat16)
    return jnp.dot(hidden, down_weight, preferred_element_type=jnp.float32)


def in_hbm(array):
    return pltpu.with_memory_space_constraint(array, pltpu.HBM)


def prepare_kernel(count, place, *refs):
    sources = refs[:4]
    table = refs[4]
    outgoing = refs[5 : 5 + count]
    tokens, gain, ids, shares, sems = refs[5 + count :]
    copies = [
        pltpu.make_async_copy(source, target, sems.at[n])
        for n, (source, target) in enumerate(
            zip(sources, (tokens, gain, ids, shares), strict=True)
        )
    ]
    for copy in copies:
        copy.start()
    for copy in copies:
        copy.wait()
    tok_rows = tokens.shape[0]
    capacity = outgoing[0].shape[0]
    values = tokens[...].astype(jnp.float32)
    scale = lax.rsqrt(jnp.mean(values * values, axis=1, keepdims=True) + rms_eps)
    normed = (values * scale * gain[...]).astype(jnp.bfloat16)
    named = []
    weighted = []
    for k in range(count):
        hit = [ids[c : c + 1, :] == (place[0] ^ k) for c in range(TOP)]
        named.append(sum(h.astype(jnp.float32) for h in hit))
        weighted.append(sum(jnp.where(h, shares[c : c + 1, :], 0.0) for c, h in enumerate(hit)))
    half = tok_rows // 2
    blank = jnp.zeros((half - count, tok_rows), jnp.float32)
    named = jnp.concatenate(named + [blank], axis=0)
    upto = lax.broadcasted_iota(jnp.int32, (tok_rows, tok_rows), 0) <= lax.broadcasted_iota(
        jnp.int32, (tok_rows, tok_rows), 1
    )
    ranks = jnp.dot(
        named.astype(jnp.bfloat16),
        upto.astype(jnp.bfloat16),
        preferred_element_type=jnp.float32,
    )
    slots = jnp.where(named > 0.5, ranks - 1.0, -1.0)
    table[...] = jnp.concatenate([slots] + weighted + [blank], axis=0).T
    spots = lax.broadcasted_iota(jnp.int32, (capacity, tok_rows), 0).astype(jnp.float32)
    for k in reversed(range(count)):
        placing = (spots == slots[k : k + 1, :]).astype(jnp.bfloat16)
        outgoing[k][...] = jnp.dot(
            placing, normed, preferred_element_type=jnp.float32
        ).astype(jnp.bfloat16)


def prepare(tokens, gain, routing_expert_index, routing_expert_weight, count, capacity):
    tok_rows, width = tokens.shape
    vmem = pl.BlockSpec(memory_space=pltpu.VMEM)
    place = lax.axis_index("ep").astype(jnp.int32).reshape(1)
    return pl.pallas_call(
        lambda *refs: prepare_kernel(count, *refs),
        in_specs=[pl.BlockSpec(memory_space=pltpu.SMEM)]
        + [pl.BlockSpec(memory_space=pltpu.HBM)] * 4,
        out_specs=[vmem] * (count + 1),
        out_shape=[jax.ShapeDtypeStruct((tok_rows, tok_rows), jnp.float32)]
        + [jax.ShapeDtypeStruct((capacity, width), jnp.bfloat16)] * count,
        scratch_shapes=[
            pltpu.VMEM((tok_rows, width), jnp.bfloat16),
            pltpu.VMEM((1, width), jnp.float32),
            pltpu.VMEM((TOP, tok_rows), jnp.int32),
            pltpu.VMEM((TOP, tok_rows), jnp.float32),
            pltpu.SemaphoreType.DMA((4,)),
        ],
        compiler_params=pltpu.CompilerParams(vmem_limit_bytes=16 * 1024 * 1024),
    )(
        place,
        in_hbm(tokens),
        in_hbm(gain.reshape(1, width)),
        in_hbm(routing_expert_index.T),
        in_hbm(routing_expert_weight.T),
    )


def combine_kernel(count, table, *refs):
    returned = refs[: count + 1]
    out, stacked = refs[count + 1 :]
    tok_rows = out.shape[0]
    half = tok_rows // 2
    capacity = returned[0].shape[0]
    local = returned[0][...].astype(jnp.float32) + returned[count][...].astype(jnp.float32)
    stacked[0:capacity, :] = local.astype(jnp.bfloat16)
    for k in range(1, count):
        stacked[k * capacity : (k + 1) * capacity, :] = returned[k][...]
    spots = lax.broadcasted_iota(jnp.int32, (tok_rows, count * capacity), 1).astype(jnp.float32)
    weights = jnp.zeros((tok_rows, count * capacity), jnp.float32)
    for k in range(count):
        slot = table[:, k : k + 1]
        aim = jnp.where(slot >= 0.0, slot + float(k * capacity), -1.0)
        weights = jnp.where(spots == aim, table[:, half + k : half + k + 1], weights)
    high = weights.astype(jnp.bfloat16)
    low = (weights - high.astype(jnp.float32)).astype(jnp.bfloat16)
    both = jnp.dot(
        jnp.concatenate([high, low], axis=0), stacked[...], preferred_element_type=jnp.float32
    )
    out[...] = (both[:tok_rows] + both[tok_rows:]).astype(jnp.bfloat16)


def combine_rows(table, returned):
    count = len(returned) - 1
    capacity, width = returned[0].shape
    vmem = pl.BlockSpec(memory_space=pltpu.VMEM)
    return pl.pallas_call(
        lambda *refs: combine_kernel(count, *refs),
        in_specs=[vmem] * (count + 2),
        out_specs=vmem,
        out_shape=jax.ShapeDtypeStruct((table.shape[0], width), jnp.bfloat16),
        scratch_shapes=[pltpu.VMEM((count * capacity, width), jnp.bfloat16)],
        compiler_params=pltpu.CompilerParams(vmem_limit_bytes=16 * 1024 * 1024),
    )(table, *returned)


def expert_kernel(*refs):
    pieces = refs[:4]
    gate, up, down = refs[4:7]
    outs = refs[7:10]
    rows, hidden, gate_here, up_here, down_here, sems = refs[10:]
    copies = [
        pltpu.make_async_copy(gate.at[0], gate_here, sems.at[0]),
        pltpu.make_async_copy(up.at[0], up_here, sems.at[1]),
        pltpu.make_async_copy(down.at[0], down_here, sems.at[2]),
    ]
    for copy in copies:
        copy.start()
    at = 0
    for piece in pieces:
        rows[at : at + piece.shape[0], :] = piece[...]
        at += piece.shape[0]
    copies[0].wait()
    gate_act = jnp.dot(rows[...], gate_here[...], preferred_element_type=jnp.float32)
    copies[1].wait()
    up_act = jnp.dot(rows[...], up_here[...], preferred_element_type=jnp.float32)
    hidden[...] = (gate_act / (1.0 + jnp.exp(-gate_act)) * up_act).astype(jnp.bfloat16)
    copies[2].wait()
    parts = jnp.dot(hidden[...], down_here[...], preferred_element_type=jnp.float32)
    at = 0
    for out in outs:
        out[...] = parts[at : at + out.shape[0]].astype(jnp.bfloat16)
        at += out.shape[0]


def expert_rows(pieces, gate, up, down):
    count, width = pieces[0].shape
    inner = gate.shape[-1]
    vmem = pl.BlockSpec(memory_space=pltpu.VMEM)
    hbm = pl.BlockSpec(memory_space=pltpu.HBM)
    return pl.pallas_call(
        expert_kernel,
        in_specs=[vmem] * 4 + [hbm] * 3,
        out_specs=[vmem] * 3,
        out_shape=[
            jax.ShapeDtypeStruct((n * count, width), jnp.bfloat16) for n in (1, 1, 2)
        ],
        scratch_shapes=[
            pltpu.VMEM((4 * count, width), jnp.bfloat16),
            pltpu.VMEM((4 * count, inner), jnp.bfloat16),
            pltpu.VMEM((width, inner), jnp.bfloat16),
            pltpu.VMEM((width, inner), jnp.bfloat16),
            pltpu.VMEM((inner, width), jnp.bfloat16),
            pltpu.SemaphoreType.DMA((3,)),
        ],
        compiler_params=pltpu.CompilerParams(vmem_limit_bytes=32 * 1024 * 1024),
        cost_estimate=pl.CostEstimate(
            flops=24 * count * width * inner,
            bytes_accessed=6 * width * inner,
            transcendentals=4 * count * inner,
        ),
    )(*pieces, *(in_hbm(w) for w in (gate, up, down)))


def added(first, second):
    total = first.astype(jnp.float32) + second.astype(jnp.float32)
    return total.astype(jnp.bfloat16)


def near_sum_kernel(keep, send, pair, kept, sent):
    rows = keep.shape[0]
    kept[...] = added(keep[...], pair[:rows])
    sent[...] = added(send[...], pair[rows:])


def far_sum_kernel(keep, other, out):
    out[...] = added(keep[...], other[...])


def sums(kernel, outputs, *rows):
    vmem = pl.BlockSpec(memory_space=pltpu.VMEM)
    return pl.pallas_call(
        kernel,
        in_specs=[vmem] * len(rows),
        out_specs=[vmem] * outputs,
        out_shape=[jax.ShapeDtypeStruct(rows[0].shape, jnp.bfloat16)] * outputs,
        compiler_params=pltpu.CompilerParams(vmem_limit_bytes=8 * 1024 * 1024),
    )(*rows)


def expert_pairs(
    second_batch_tokens,
    expert_norm_gain,
    routing_expert_index,
    routing_expert_weight,
    gate,
    up,
    down,
):
    experts = lax.axis_size("ep")
    tok_rows = second_batch_tokens.shape[0]
    capacity = max(2, 5 * tok_rows * TOP // (4 * experts))
    table, *outgoing = prepare(
        second_batch_tokens,
        expert_norm_gain,
        routing_expert_index,
        routing_expert_weight,
        experts,
        capacity,
    )
    far, near = 2, 1
    returned = [None] * experts + [None]
    for k in reversed(range(experts)):
        own = swap(outgoing[k], "ep", k) if k else outgoing[k]
        across = swap(own, "tp", far)
        beside = swap(own, "tp", near)
        corner = swap(across, "tp", near)
        pieces = (own, across, beside, corner)
        keep, send, pair = expert_rows(pieces, gate, up, down)
        pair = swap(pair, "tp", near)
        keep, send = sums(near_sum_kernel, 2, keep, send, pair)
        other = swap(send, "tp", far)
        if k:
            total = sums(far_sum_kernel, 1, keep, other)[0]
            returned[k] = swap(total, "ep", k)
        else:
            returned[0] = keep
            returned[experts] = other
    return combine_rows(table, returned)


def expert_branch(
    second_batch_tokens,
    expert_norm_gain,
    routing_expert_index,
    routing_expert_weight,
    gate,
    up,
    down,
):
    tok_rows = second_batch_tokens.shape[0]
    experts = lax.axis_size("ep")
    capacity = max(2, 5 * tok_rows * TOP // (4 * experts))
    tokens_f = second_batch_tokens.astype(jnp.float32)
    normed = (
        tokens_f
        * lax.rsqrt(jnp.mean(tokens_f * tokens_f, axis=1, keepdims=True) + rms_eps)
        * expert_norm_gain
    ).astype(jnp.bfloat16)
    ids = jnp.arange(experts, dtype=jnp.int32)
    hits = routing_expert_index[:, :, None] == ids[None, None, :]
    named = jnp.any(hits, axis=1)
    share = jnp.sum(jnp.where(hits, routing_expert_weight[:, :, None], 0.0), axis=1)
    upto = jnp.tril(jnp.ones((tok_rows, tok_rows), jnp.bfloat16))
    ranks = jnp.dot(upto, named.astype(jnp.bfloat16), preferred_element_type=jnp.float32)
    slot = jnp.where(named, ranks.astype(jnp.int32) - 1, -1)
    spots = jnp.arange(capacity, dtype=jnp.int32)
    placing = (slot.T[:, None, :] == spots[None, :, None]).astype(jnp.bfloat16)
    combine = jnp.where(slot[:, :, None] == spots[None, None, :], share[:, :, None], 0.0)
    outgoing = jnp.dot(
        placing.reshape(experts * capacity, tok_rows),
        normed,
        preferred_element_type=jnp.float32,
    ).astype(jnp.bfloat16)
    arrived = lax.all_to_all(outgoing, "ep", split_axis=0, concat_axis=0, tiled=True)
    row_block = lax.all_gather(arrived, "tp", axis=0, tiled=True)
    terms = expert_part(row_block, gate[0], up[0], down[0]).astype(jnp.bfloat16)
    summed = lax.psum_scatter(terms, "tp", scatter_dimension=0, tiled=True)
    returned = lax.all_to_all(summed, "ep", split_axis=0, concat_axis=0, tiled=True)
    combine = combine.reshape(tok_rows, experts * capacity)
    high = combine.astype(jnp.bfloat16)
    low = (combine - high.astype(jnp.float32)).astype(jnp.bfloat16)
    both = jnp.dot(
        jnp.concatenate([high, low], axis=0), returned, preferred_element_type=jnp.float32
    )
    return (both[:tok_rows] + both[tok_rows:]).astype(jnp.bfloat16)


def is_paired(experts, shards):
    return experts == 4 and shards == 4


def on_device(
    memory_query_rows,
    memory_key_rows,
    memory_value_rows,
    input_gate_log,
    forget_gate_logits,
    forget_log_extra,
    memory_output_weight,
    second_batch_tokens,
    expert_norm_gain,
    routing_expert_index,
    routing_expert_weight,
    expert_gate_matrix,
    expert_up_matrix,
    expert_down_matrix,
):
    paired = is_paired(lax.axis_size("ep"), lax.axis_size("tp"))
    paired = paired and input_gate_log.shape[1] == BLOCK
    expert_out = (expert_pairs if paired else expert_branch)(
        second_batch_tokens,
        expert_norm_gain,
        routing_expert_index,
        routing_expert_weight,
        expert_gate_matrix,
        expert_up_matrix,
        expert_down_matrix,
    )
    mixed_out = (memory_pairs if paired else memory_branch)(
        memory_query_rows,
        memory_key_rows,
        memory_value_rows,
        input_gate_log,
        forget_gate_logits,
        forget_log_extra,
        memory_output_weight,
    )
    return (mixed_out, expert_out)


def solution(mesh):
    placed = (
        P(("grp", "ep"), "tp"),
        P(("grp", "ep"), "tp"),
        P(("grp", "ep"), "tp"),
        P("tp", ("grp", "ep")),
        P("tp", ("grp", "ep")),
        P("tp", ("grp", "ep")),
        P(None, "tp"),
        P(("grp", "ep", "tp"), None),
        P(),
        P(("grp", "ep", "tp"), None),
        P(("grp", "ep", "tp"), None),
        P("ep", None, "tp"),
        P("ep", None, "tp"),
        P("ep", "tp", None),
    )
    return jax.shard_map(
        on_device,
        mesh=mesh,
        in_specs=placed,
        out_specs=(P(("grp", "ep"), "tp"), P(("grp", "ep", "tp"), None)),
        check_vma=False,
    )
```

```python
import jax
import jax.numpy as jnp
from jax import lax
from jax.experimental import pallas as pl
from jax.experimental.pallas import tpu as pltpu
from jax.sharding import PartitionSpec as P

DH = 128
TOP = 2
BLOCK = 128


neg_big = -1e30
rms_eps = 1e-06
highest = lax.Precision.HIGHEST


def entering(part, axis, combine, identity):
    place = lax.axis_index(axis)
    gathered = jax.tree.map(lambda a: lax.all_gather(a, axis), part)
    state = jax.tree.map(lambda a, e: jnp.zeros_like(a) + jnp.asarray(e, a.dtype), part, identity)

    def one(turn, state):
        return combine(
            state, jax.tree.map(lambda a: lax.dynamic_index_in_dim(a, turn, 0, False), gathered)
        )

    return lax.fori_loop(0, place, one, state)


def state_update(state_in, inputs, cumulative):
    memory, normer, stabilizer = state_in
    key_rows, values, in_gate, _ = inputs
    block_total = cumulative[:, -1]
    weights = block_total[:, None] - cumulative + in_gate
    new_stab = jnp.maximum(block_total + stabilizer, jnp.max(weights, axis=-1))
    scaled = jnp.exp(weights - new_stab[:, None])
    retained = jnp.exp(block_total + stabilizer - new_stab)
    weighted_keys = scaled[:, :, None] * key_rows
    memory = retained[:, None, None] * memory + jnp.einsum(
        "hsd,hse->hde", weighted_keys, values, precision=highest
    )
    normer = retained[:, None] * normer + jnp.sum(weighted_keys, axis=1)
    return (memory, normer, new_stab)


def block_step(state_in, inputs, cumulative):
    memory, normer, stabilizer = state_in
    queries, key_rows, values, in_gate, _ = inputs
    length = queries.shape[1]
    causal = jnp.tril(jnp.ones((length, length), dtype=bool))
    decays = jnp.where(
        causal, cumulative[:, :, None] - cumulative[:, None, :] + in_gate[:, None, :], -jnp.inf
    )
    carried_max = cumulative + stabilizer[:, None]
    row_max = jnp.maximum(jnp.max(decays, axis=-1), carried_max)
    scores = jnp.einsum("htd,hsd->hts", queries, key_rows, precision=highest) * jnp.exp(
        decays - row_max[:, :, None]
    )
    carried = jnp.exp(carried_max - row_max)
    numerator = carried[:, :, None] * jnp.einsum(
        "htd,hde->hte", queries, memory, precision=highest
    ) + jnp.einsum("hts,hse->hte", scores, values, precision=highest)
    denominator = carried * jnp.einsum("htd,hd->ht", queries, normer, precision=highest) + jnp.sum(
        scores, axis=-1
    )
    return numerator / jnp.maximum(jnp.abs(denominator), jnp.exp(-row_max))[:, :, None]


def join_states(earlier, later, total_late):
    mem_early, norm_early, stab_early = earlier
    mem_late, norm_late, stab_late = later
    stabilizer = jnp.maximum(total_late + stab_early, stab_late)
    early_scale = jnp.exp(total_late + stab_early - stabilizer)
    late_scale = jnp.exp(stab_late - stabilizer)
    memory = early_scale[:, None, None] * mem_early + late_scale[:, None, None] * mem_late
    normer = early_scale[:, None] * norm_early + late_scale[:, None] * norm_late
    return (memory, normer, stabilizer)


def join_totals(earlier, later):
    joined = join_states(earlier[:3], later[:3], later[3])
    return joined + (earlier[3] + later[3],)


def split_blocks(row_block, heads):
    count = row_block.shape[0] // BLOCK
    return row_block.astype(jnp.float32).reshape(count, BLOCK, heads, -1).transpose(0, 2, 1, 3)


def gate_blocks(gate_rows):
    heads = gate_rows.shape[0]
    return gate_rows.reshape(heads, -1, BLOCK).transpose(1, 0, 2)


def swap(rows, axis, bit):
    size = lax.axis_size(axis)
    return lax.ppermute(rows, axis, [(i, i ^ bit) for i in range(size)])


def tp_bits():
    size = lax.axis_size("tp")
    bits = []
    while size > 1:
        size //= 2
        bits.append(size)
    return bits


def gather_columns(rows):
    place = lax.axis_index("tp")
    for bit in reversed(tp_bits()):
        other = swap(rows, "tp", bit)
        upper = (place & bit) != 0
        rows = jnp.concatenate(
            [jnp.where(upper, other, rows), jnp.where(upper, rows, other)], axis=1
        )
    return rows


def memory_branch(
    memory_query_rows,
    memory_key_rows,
    memory_value_rows,
    input_gate_log,
    forget_gate_logits,
    forget_log_extra,
    memory_output_weight,
):
    heads_local, positions = input_gate_log.shape
    queries = split_blocks(memory_query_rows, heads_local)
    key_rows = split_blocks(memory_key_rows, heads_local) * DH ** (-0.5)
    values = split_blocks(memory_value_rows, heads_local)
    in_gate = gate_blocks(input_gate_log)
    forget_log_value = jax.nn.log_sigmoid(forget_gate_logits) + forget_log_extra
    forget = gate_blocks(forget_log_value)
    upto = jnp.triu(jnp.ones((BLOCK, BLOCK), jnp.float32))
    cumulative = jnp.einsum("bhs,st->bht", forget, upto, precision=highest)
    zero_memory = jnp.zeros((heads_local, DH, DH), jnp.float32)
    zero_normer = jnp.zeros((heads_local, DH), jnp.float32)
    low_stab = jnp.full((heads_local,), neg_big, jnp.float32)
    count = positions // BLOCK
    state = (zero_memory, zero_normer, low_stab)
    for b in range(count):
        state = state_update(state, (key_rows[b], values[b], in_gate[b], forget[b]), cumulative[b])
    totals = jnp.sum(cumulative[:, :, -1], axis=0)
    identity = (zero_memory, zero_normer, low_stab, jnp.zeros((heads_local,), jnp.float32))
    mem_prior, norm_prior, stab_prior, total_prior = entering(
        state + (totals,), "ep", join_totals, identity
    )
    stab_in = jnp.maximum(total_prior, stab_prior)
    factor = jnp.exp(stab_prior - stab_in)
    incoming = (factor[:, None, None] * mem_prior, factor[:, None] * norm_prior, stab_in)
    outputs = []
    for b in range(count):
        block = (queries[b], key_rows[b], values[b], in_gate[b], forget[b])
        outputs.append(block_step(incoming, block, cumulative[b]))
        if b + 1 < count:
            incoming = state_update(incoming, block[1:], cumulative[b])
    memory_rows = (
        jnp.stack(outputs).transpose(0, 2, 1, 3).reshape(positions, -1).astype(jnp.bfloat16)
    )
    mixed = jnp.dot(
        gather_columns(memory_rows), memory_output_weight, preferred_element_type=jnp.float32
    )
    return mixed.astype(jnp.bfloat16)


def split_terms(array):
    high = array.astype(jnp.bfloat16)
    return high, (array - high.astype(jnp.float32)).astype(jnp.bfloat16)


def wide_dot(left, right):
    high, low = split_terms(left)
    both = jnp.dot(
        jnp.concatenate([high, low], axis=0), right, preferred_element_type=jnp.float32
    )
    return both[: left.shape[0]] + both[left.shape[0] :]


def local_kernel(*refs):
    sources = refs[:6]
    local, after, inside, columns = refs[6:10]
    query, key, value, gate, logits, extra, sems = refs[10:]
    copies = [
        pltpu.make_async_copy(source, target, sems.at[n])
        for n, (source, target) in enumerate(zip(sources, refs[10:16], strict=True))
    ]
    for copy in copies:
        copy.start()
    for copy in copies:
        copy.wait()
    heads = gate.shape[0]
    size = query.shape[0]
    scale = DH ** (-0.5)
    raw = logits[...]
    forget = jnp.minimum(raw, 0.0) - jnp.log1p(jnp.exp(-jnp.abs(raw))) + extra[...]
    first = lax.broadcasted_iota(jnp.int32, (size, size), 0)
    second = lax.broadcasted_iota(jnp.int32, (size, size), 1)
    upto = (first <= second).astype(jnp.float32)
    cumulative = jnp.dot(forget, upto, precision=highest, preferred_element_type=jnp.float32)
    ending = cumulative[:, size - 1 : size] - cumulative + gate[...]
    peak = jnp.max(ending, axis=1, keepdims=True)
    grow = jnp.exp(ending - peak)
    blank = jnp.zeros((size - 2 * heads, size), jnp.float32)
    turned = jnp.concatenate([cumulative, grow, blank], axis=0).T
    notes = [jnp.zeros((size, size - 3 * heads), jnp.float32)]
    for h in range(heads):
        span = slice(h * DH, (h + 1) * DH)
        queries = query[:, span]
        keys = key[:, span]
        values = value[:, span]
        keys_f = keys.astype(jnp.float32) * scale
        weighted = keys_f.T * grow[h : h + 1, :]
        memory = wide_dot(weighted, values)
        normer = jnp.sum(keys_f * turned[:, heads + h : heads + h + 1], axis=0, keepdims=True)
        total = cumulative[h : h + 1, size - 1 : size]
        stab = peak[h : h + 1, :]
        later = jnp.maximum(total, stab)
        ratio = jnp.exp(stab - later)
        local[h, 0:DH, :] = memory
        local[h, DH : DH + 1, :] = normer
        local[h, DH + 1 : DH + 2, :] = jnp.broadcast_to(stab, (1, DH))
        local[h, DH + 2 : DH + 3, :] = jnp.broadcast_to(total, (1, DH))
        after[h, 0:DH, :] = memory * ratio
        after[h, DH : DH + 1, :] = normer * ratio
        after[h, DH + 1 : DH + 2, :] = jnp.broadcast_to(later, (1, DH))
        column = turned[:, h : h + 1]
        decays = column - cumulative[h : h + 1, :] + gate[h : h + 1, :]
        decays = jnp.where(second <= first, decays, -jnp.inf)
        row_max = jnp.max(decays, axis=1, keepdims=True)
        scores = lax.dot_general(
            queries, keys, (((1,), (1,)), ((), ())), preferred_element_type=jnp.float32
        )
        scores = scores * scale * jnp.exp(decays - row_max)
        inside[:, span] = wide_dot(scores, values)
        notes = notes[:-1] + [column, row_max, jnp.sum(scores, axis=1, keepdims=True)] + notes[-1:]
    columns[...] = jnp.concatenate(notes, axis=1)


def join_kernel(local, *refs):
    earlier = refs[:-1]
    after = refs[-1]
    for h in range(local.shape[0]):
        entering = sum(part[h] for part in earlier)
        stab = entering[DH + 1 : DH + 2, :] + local[h, DH + 2 : DH + 3, :]
        late = local[h, DH + 1 : DH + 2, :]
        later = jnp.maximum(stab, late)
        keep = jnp.exp(stab - later)
        grow = jnp.exp(late - later)
        after[h, 0 : DH + 1, :] = entering[0 : DH + 1, :] * keep + local[h, 0 : DH + 1, :] * grow
        after[h, DH + 1 : DH + 2, :] = later


def output_kernel(query, inside, columns, *refs):
    earlier = refs[:-1]
    out = refs[-1]
    for h in range(earlier[0].shape[0]):
        span = slice(h * DH, (h + 1) * DH)
        entering = sum(part[h] for part in earlier)
        queries = query[:, span]
        high, low = split_terms(entering[0:DH, :])
        carried = jnp.dot(queries, high, preferred_element_type=jnp.float32) + jnp.dot(
            queries, low, preferred_element_type=jnp.float32
        )
        normed = jnp.sum(
            queries.astype(jnp.float32) * entering[DH : DH + 1, :], axis=1, keepdims=True
        )
        arrived = columns[:, 3 * h : 3 * h + 1] + entering[DH + 1 : DH + 2, 0:1]
        row_max = columns[:, 3 * h + 1 : 3 * h + 2]
        top = jnp.maximum(row_max, arrived)
        outer = jnp.exp(arrived - top)
        inner = jnp.exp(row_max - top)
        below = outer * normed + inner * columns[:, 3 * h + 2 : 3 * h + 3]
        above = outer * carried + inner * inside[:, span]
        out[:, span] = (above / jnp.maximum(jnp.abs(below), jnp.exp(-top))).astype(jnp.bfloat16)


def mixed_kernel(place, own, across, beside, corner, weight, out):
    width = own.shape[1]
    total = jnp.zeros(out.shape, jnp.float32)
    for mask, part in ((0, own), (2, across), (1, beside), (3, corner)):
        rows = pl.ds(pl.multiple_of((place[0] ^ mask) * width, width), width)
        total += jnp.dot(part[...], weight[rows, :], preferred_element_type=jnp.float32)
    out[...] = total.astype(jnp.bfloat16)


def memory_pairs(
    memory_query_rows,
    memory_key_rows,
    memory_value_rows,
    input_gate_log,
    forget_gate_logits,
    forget_log_extra,
    memory_output_weight,
):
    heads = input_gate_log.shape[0]
    size, width = memory_query_rows.shape
    vmem = pl.BlockSpec(memory_space=pltpu.VMEM)
    params = pltpu.CompilerParams(vmem_limit_bytes=8 * 1024 * 1024)
    packed = jax.ShapeDtypeStruct((heads, DH + 8, DH), jnp.float32)
    local, after, inside, columns = pl.pallas_call(
        local_kernel,
        in_specs=[pl.BlockSpec(memory_space=pltpu.HBM)] * 6,
        out_specs=[vmem] * 4,
        out_shape=[
            packed,
            packed,
            jax.ShapeDtypeStruct((size, width), jnp.float32),
            jax.ShapeDtypeStruct((size, size), jnp.float32),
        ],
        scratch_shapes=[pltpu.VMEM((size, width), jnp.bfloat16)] * 3
        + [pltpu.VMEM((heads, size), jnp.float32)] * 3
        + [pltpu.SemaphoreType.DMA((6,))],
        compiler_params=params,
    )(
        in_hbm(memory_query_rows),
        in_hbm(memory_key_rows),
        in_hbm(memory_value_rows),
        in_hbm(input_gate_log),
        in_hbm(forget_gate_logits),
        in_hbm(forget_log_extra),
    )
    earlier = []
    hops = lax.axis_size("ep") - 1
    for hop in range(hops):
        if hop:
            after = pl.pallas_call(
                join_kernel,
                in_specs=[vmem] * (1 + hop),
                out_specs=vmem,
                out_shape=packed,
                compiler_params=params,
            )(local, *earlier)
        earlier.append(lax.ppermute(after, "ep", [(hop, hop + 1)]))
    own = pl.pallas_call(
        output_kernel,
        in_specs=[vmem] * (3 + hops),
        out_specs=vmem,
        out_shape=jax.ShapeDtypeStruct((size, width), jnp.bfloat16),
        compiler_params=params,
    )(memory_query_rows, inside, columns, *earlier)
    across = swap(own, "tp", 2)
    beside = swap(own, "tp", 1)
    corner = swap(across, "tp", 1)
    place = lax.axis_index("tp").astype(jnp.int32).reshape(1)
    return pl.pallas_call(
        mixed_kernel,
        in_specs=[pl.BlockSpec(memory_space=pltpu.SMEM)] + [vmem] * 5,
        out_specs=vmem,
        out_shape=jax.ShapeDtypeStruct((size, memory_output_weight.shape[1]), jnp.bfloat16),
        compiler_params=params,
    )(place, own, across, beside, corner, memory_output_weight)


def expert_part(rows, gate_weight, up_weight, down_weight):
    gate_act = jnp.dot(rows, gate_weight, preferred_element_type=jnp.float32)
    up_act = jnp.dot(rows, up_weight, preferred_element_type=jnp.float32)
    hidden = (jax.nn.silu(gate_act) * up_act).astype(jnp.bfloat16)
    return jnp.dot(hidden, down_weight, preferred_element_type=jnp.float32)


def in_hbm(array):
    return pltpu.with_memory_space_constraint(array, pltpu.HBM)


def prepare_kernel(count, place, *refs):
    sources = refs[:4]
    table = refs[4]
    outgoing = refs[5 : 5 + count]
    tokens, gain, ids, shares, sems = refs[5 + count :]
    copies = [
        pltpu.make_async_copy(source, target, sems.at[n])
        for n, (source, target) in enumerate(
            zip(sources, (tokens, gain, ids, shares), strict=True)
        )
    ]
    for copy in copies:
        copy.start()
    for copy in copies:
        copy.wait()
    tok_rows = tokens.shape[0]
    capacity = outgoing[0].shape[0]
    values = tokens[...].astype(jnp.float32)
    scale = lax.rsqrt(jnp.mean(values * values, axis=1, keepdims=True) + rms_eps)
    normed = (values * scale * gain[...]).astype(jnp.bfloat16)
    named = []
    weighted = []
    for k in range(count):
        hit = [ids[c : c + 1, :] == (place[0] ^ k) for c in range(TOP)]
        named.append(sum(h.astype(jnp.float32) for h in hit))
        weighted.append(sum(jnp.where(h, shares[c : c + 1, :], 0.0) for c, h in enumerate(hit)))
    half = tok_rows // 2
    blank = jnp.zeros((half - count, tok_rows), jnp.float32)
    named = jnp.concatenate(named + [blank], axis=0)
    upto = lax.broadcasted_iota(jnp.int32, (tok_rows, tok_rows), 0) <= lax.broadcasted_iota(
        jnp.int32, (tok_rows, tok_rows), 1
    )
    ranks = jnp.dot(
        named.astype(jnp.bfloat16),
        upto.astype(jnp.bfloat16),
        preferred_element_type=jnp.float32,
    )
    slots = jnp.where(named > 0.5, ranks - 1.0, -1.0)
    table[...] = jnp.concatenate([slots] + weighted + [blank], axis=0).T
    spots = lax.broadcasted_iota(jnp.int32, (capacity, tok_rows), 0).astype(jnp.float32)
    for k in reversed(range(count)):
        placing = (spots == slots[k : k + 1, :]).astype(jnp.bfloat16)
        outgoing[k][...] = jnp.dot(
            placing, normed, preferred_element_type=jnp.float32
        ).astype(jnp.bfloat16)


def prepare(tokens, gain, routing_expert_index, routing_expert_weight, count, capacity):
    tok_rows, width = tokens.shape
    vmem = pl.BlockSpec(memory_space=pltpu.VMEM)
    place = lax.axis_index("ep").astype(jnp.int32).reshape(1)
    return pl.pallas_call(
        lambda *refs: prepare_kernel(count, *refs),
        in_specs=[pl.BlockSpec(memory_space=pltpu.SMEM)]
        + [pl.BlockSpec(memory_space=pltpu.HBM)] * 4,
        out_specs=[vmem] * (count + 1),
        out_shape=[jax.ShapeDtypeStruct((tok_rows, tok_rows), jnp.float32)]
        + [jax.ShapeDtypeStruct((capacity, width), jnp.bfloat16)] * count,
        scratch_shapes=[
            pltpu.VMEM((tok_rows, width), jnp.bfloat16),
            pltpu.VMEM((1, width), jnp.float32),
            pltpu.VMEM((TOP, tok_rows), jnp.int32),
            pltpu.VMEM((TOP, tok_rows), jnp.float32),
            pltpu.SemaphoreType.DMA((4,)),
        ],
        compiler_params=pltpu.CompilerParams(vmem_limit_bytes=16 * 1024 * 1024),
    )(
        place,
        in_hbm(tokens),
        in_hbm(gain.reshape(1, width)),
        in_hbm(routing_expert_index.T),
        in_hbm(routing_expert_weight.T),
    )


def combine_kernel(count, table, *refs):
    returned = refs[: count + 1]
    out, stacked = refs[count + 1 :]
    tok_rows = out.shape[0]
    half = tok_rows // 2
    capacity = returned[0].shape[0]
    local = returned[0][...].astype(jnp.float32) + returned[count][...].astype(jnp.float32)
    stacked[0:capacity, :] = local.astype(jnp.bfloat16)
    for k in range(1, count):
        stacked[k * capacity : (k + 1) * capacity, :] = returned[k][...]
    spots = lax.broadcasted_iota(jnp.int32, (tok_rows, count * capacity), 1).astype(jnp.float32)
    weights = jnp.zeros((tok_rows, count * capacity), jnp.float32)
    for k in range(count):
        slot = table[:, k : k + 1]
        aim = jnp.where(slot >= 0.0, slot + float(k * capacity), -1.0)
        weights = jnp.where(spots == aim, table[:, half + k : half + k + 1], weights)
    high = weights.astype(jnp.bfloat16)
    low = (weights - high.astype(jnp.float32)).astype(jnp.bfloat16)
    both = jnp.dot(
        jnp.concatenate([high, low], axis=0), stacked[...], preferred_element_type=jnp.float32
    )
    out[...] = (both[:tok_rows] + both[tok_rows:]).astype(jnp.bfloat16)


def combine_rows(table, returned):
    count = len(returned) - 1
    capacity, width = returned[0].shape
    vmem = pl.BlockSpec(memory_space=pltpu.VMEM)
    return pl.pallas_call(
        lambda *refs: combine_kernel(count, *refs),
        in_specs=[vmem] * (count + 2),
        out_specs=vmem,
        out_shape=jax.ShapeDtypeStruct((table.shape[0], width), jnp.bfloat16),
        scratch_shapes=[pltpu.VMEM((count * capacity, width), jnp.bfloat16)],
        compiler_params=pltpu.CompilerParams(vmem_limit_bytes=16 * 1024 * 1024),
    )(table, *returned)


def load_kernel(gate, up, down, gate_here, up_here, down_here, sems):
    copies = [
        pltpu.make_async_copy(source.at[0], target, sems.at[n])
        for n, (source, target) in enumerate(
            ((gate, gate_here), (up, up_here), (down, down_here))
        )
    ]
    for copy in copies:
        copy.start()
    for copy in copies:
        copy.wait()


def load_weights(*weights):
    hbm = pl.BlockSpec(memory_space=pltpu.HBM)
    vmem = pl.BlockSpec(memory_space=pltpu.VMEM)
    return pl.pallas_call(
        load_kernel,
        in_specs=[hbm] * 3,
        out_specs=[vmem] * 3,
        out_shape=[pltpu.VMEM(w.shape[1:], w.dtype) for w in weights],
        scratch_shapes=[pltpu.SemaphoreType.DMA((3,))],
        compiler_params=pltpu.CompilerParams(vmem_limit_bytes=16 * 1024 * 1024),
    )(*(in_hbm(w) for w in weights))


def expert_kernel(first, second, gate, up, down, first_out, second_out, rows, hidden):
    count = first.shape[0]
    rows[:count, :] = first[...]
    rows[count:, :] = second[...]
    gate_act = jnp.dot(rows[...], gate[...], preferred_element_type=jnp.float32)
    up_act = jnp.dot(rows[...], up[...], preferred_element_type=jnp.float32)
    hidden[...] = (gate_act / (1.0 + jnp.exp(-gate_act)) * up_act).astype(jnp.bfloat16)
    parts = jnp.dot(hidden[...], down[...], preferred_element_type=jnp.float32)
    first_out[...] = parts[:count].astype(jnp.bfloat16)
    second_out[...] = parts[count:].astype(jnp.bfloat16)


def expert_rows(first, second, weights):
    count, width = first.shape
    inner = weights[0].shape[-1]
    vmem = pl.BlockSpec(memory_space=pltpu.VMEM)
    here = [pltpu.with_memory_space_constraint(w, pltpu.VMEM) for w in weights]
    return pl.pallas_call(
        expert_kernel,
        in_specs=[vmem] * 5,
        out_specs=[vmem] * 2,
        out_shape=[jax.ShapeDtypeStruct((count, width), jnp.bfloat16)] * 2,
        scratch_shapes=[
            pltpu.VMEM((2 * count, width), jnp.bfloat16),
            pltpu.VMEM((2 * count, inner), jnp.bfloat16),
        ],
        compiler_params=pltpu.CompilerParams(vmem_limit_bytes=24 * 1024 * 1024),
        cost_estimate=pl.CostEstimate(
            flops=12 * count * width * inner,
            bytes_accessed=8 * count * width,
            transcendentals=2 * count * inner,
        ),
    )(first, second, *here)


def added(first, second):
    total = first.astype(jnp.float32) + second.astype(jnp.float32)
    return total.astype(jnp.bfloat16)


def sum_kernel(first, second, out):
    out[...] = added(first[...], second[...])


def summed(first, second):
    vmem = pl.BlockSpec(memory_space=pltpu.VMEM)
    return pl.pallas_call(
        sum_kernel,
        in_specs=[vmem] * 2,
        out_specs=vmem,
        out_shape=jax.ShapeDtypeStruct(first.shape, jnp.bfloat16),
        compiler_params=pltpu.CompilerParams(vmem_limit_bytes=8 * 1024 * 1024),
    )(first, second)


def expert_pairs(
    second_batch_tokens,
    expert_norm_gain,
    routing_expert_index,
    routing_expert_weight,
    gate,
    up,
    down,
):
    experts = lax.axis_size("ep")
    tok_rows = second_batch_tokens.shape[0]
    capacity = max(2, 5 * tok_rows * TOP // (4 * experts))
    table, *outgoing = prepare(
        second_batch_tokens,
        expert_norm_gain,
        routing_expert_index,
        routing_expert_weight,
        experts,
        capacity,
    )
    far, near = 2, 1
    weights = load_weights(gate, up, down)
    returned = [None] * experts + [None]
    for k in reversed(range(experts)):
        own = swap(outgoing[k], "ep", k) if k else outgoing[k]
        if k == 1:
            across = swap(swap(outgoing[k], "tp", far), "ep", k)
        else:
            across = swap(own, "tp", far)
        beside = swap(own, "tp", near)
        corner = swap(across, "tp", near)
        keep, near_part = expert_rows(own, beside, weights)
        send, far_part = expert_rows(across, corner, weights)
        keep_more = swap(near_part, "tp", near)
        send_more = swap(far_part, "tp", near)
        other = swap(summed(send, send_more), "tp", far)
        keep = summed(keep, keep_more)
        if k:
            returned[k] = swap(summed(keep, other), "ep", k)
        else:
            returned[0] = keep
            returned[experts] = other
    return combine_rows(table, returned)


def expert_branch(
    second_batch_tokens,
    expert_norm_gain,
    routing_expert_index,
    routing_expert_weight,
    gate,
    up,
    down,
):
    tok_rows = second_batch_tokens.shape[0]
    experts = lax.axis_size("ep")
    capacity = max(2, 5 * tok_rows * TOP // (4 * experts))
    tokens_f = second_batch_tokens.astype(jnp.float32)
    normed = (
        tokens_f
        * lax.rsqrt(jnp.mean(tokens_f * tokens_f, axis=1, keepdims=True) + rms_eps)
        * expert_norm_gain
    ).astype(jnp.bfloat16)
    ids = jnp.arange(experts, dtype=jnp.int32)
    hits = routing_expert_index[:, :, None] == ids[None, None, :]
    named = jnp.any(hits, axis=1)
    share = jnp.sum(jnp.where(hits, routing_expert_weight[:, :, None], 0.0), axis=1)
    upto = jnp.tril(jnp.ones((tok_rows, tok_rows), jnp.bfloat16))
    ranks = jnp.dot(upto, named.astype(jnp.bfloat16), preferred_element_type=jnp.float32)
    slot = jnp.where(named, ranks.astype(jnp.int32) - 1, -1)
    spots = jnp.arange(capacity, dtype=jnp.int32)
    placing = (slot.T[:, None, :] == spots[None, :, None]).astype(jnp.bfloat16)
    combine = jnp.where(slot[:, :, None] == spots[None, None, :], share[:, :, None], 0.0)
    outgoing = jnp.dot(
        placing.reshape(experts * capacity, tok_rows),
        normed,
        preferred_element_type=jnp.float32,
    ).astype(jnp.bfloat16)
    arrived = lax.all_to_all(outgoing, "ep", split_axis=0, concat_axis=0, tiled=True)
    row_block = lax.all_gather(arrived, "tp", axis=0, tiled=True)
    terms = expert_part(row_block, gate[0], up[0], down[0]).astype(jnp.bfloat16)
    summed = lax.psum_scatter(terms, "tp", scatter_dimension=0, tiled=True)
    returned = lax.all_to_all(summed, "ep", split_axis=0, concat_axis=0, tiled=True)
    combine = combine.reshape(tok_rows, experts * capacity)
    high = combine.astype(jnp.bfloat16)
    low = (combine - high.astype(jnp.float32)).astype(jnp.bfloat16)
    both = jnp.dot(
        jnp.concatenate([high, low], axis=0), returned, preferred_element_type=jnp.float32
    )
    return (both[:tok_rows] + both[tok_rows:]).astype(jnp.bfloat16)


def is_paired(experts, shards):
    return experts == 4 and shards == 4


def on_device(
    memory_query_rows,
    memory_key_rows,
    memory_value_rows,
    input_gate_log,
    forget_gate_logits,
    forget_log_extra,
    memory_output_weight,
    second_batch_tokens,
    expert_norm_gain,
    routing_expert_index,
    routing_expert_weight,
    expert_gate_matrix,
    expert_up_matrix,
    expert_down_matrix,
):
    paired = is_paired(lax.axis_size("ep"), lax.axis_size("tp"))
    paired = paired and input_gate_log.shape[1] == BLOCK
    expert_out = (expert_pairs if paired else expert_branch)(
        second_batch_tokens,
        expert_norm_gain,
        routing_expert_index,
        routing_expert_weight,
        expert_gate_matrix,
        expert_up_matrix,
        expert_down_matrix,
    )
    mixed_out = (memory_pairs if paired else memory_branch)(
        memory_query_rows,
        memory_key_rows,
        memory_value_rows,
        input_gate_log,
        forget_gate_logits,
        forget_log_extra,
        memory_output_weight,
    )
    return (mixed_out, expert_out)


def solution(mesh):
    placed = (
        P(("grp", "ep"), "tp"),
        P(("grp", "ep"), "tp"),
        P(("grp", "ep"), "tp"),
        P("tp", ("grp", "ep")),
        P("tp", ("grp", "ep")),
        P("tp", ("grp", "ep")),
        P(None, "tp"),
        P(("grp", "ep", "tp"), None),
        P(),
        P(("grp", "ep", "tp"), None),
        P(("grp", "ep", "tp"), None),
        P("ep", None, "tp"),
        P("ep", None, "tp"),
        P("ep", "tp", None),
    )
    return jax.shard_map(
        on_device,
        mesh=mesh,
        in_specs=placed,
        out_specs=(P(("grp", "ep"), "tp"), P(("grp", "ep", "tp"), None)),
        check_vma=False,
    )
```
